32 devices in a mesh: tp: 8 (over z, core), dp: 4 (over y, x).
Axes of the slice: x: 2, y: 2, z: 4, core: 2. Of those that a mesh axis runs over, the one named last changes fastest.
Arguments:
- tokens: bfloat16 [32, 4096], P('tp', 'dp'), may hold values from -30 to 30
- lengths: int32 [32], P('dp'), may hold values from 1 to 8192, 65536 in all
- in_gain: float32 [2, 4096], P(None, 'dp'), may hold values from 0.1 to 1.9
- w_recept: bfloat16 [2, 4096, 2048], P(None, 'dp', 'tp'), may hold values from -0.09375 to 0.09375
- w_key: bfloat16 [2, 4096, 2048], P(None, 'dp', 'tp'), may hold values from -0.09375 to 0.09375
- w_value: bfloat16 [2, 4096, 2048], P(None, 'dp', 'tp'), may hold values from -0.09375 to 0.09375
- w_decay: bfloat16 [2, 4096, 2048], P(None, 'dp', 'tp'), may hold values from -0.09375 to 0.09375
- w_rate: bfloat16 [2, 4096, 2048], P(None, 'dp', 'tp'), may hold values from -0.09375 to 0.09375
- w_gate: bfloat16 [2, 4096, 2048], P(None, 'dp', 'tp'), may hold values from -0.09375 to 0.09375
- w_out: bfloat16 [2, 2048, 4096], P(None, 'tp', 'dp'), may hold values from -0.125 to 0.125
- decay_base: float32 [2, 2048], P(None, 'tp'), may hold values from -6 to 6
- mix_gain: float32 [2, 2048], P(None, 'tp'), may hold values from 0.1 to 1.9
- states: float32 [2, 32, 32, 64, 64], P(None, 'dp', 'tp'), may hold values from -6 to 6
Outputs:
- next_tokens: bfloat16 [32, 4096], P('tp', 'dp')
- new_states: float32 [2, 32, 32, 64, 64], P(None, 'dp', 'tp')
The draws below stay inside these ranges and needn't reach their ends.
All inputs are finite; a program needn't handle non-finite values. No bound on the sum of `lengths` on one device may be relied on, other than what follows from the above.
Results may differ from the reference program's by a relative error of at most 0.0065.
Values may be sent and summed in bfloat16 or wider, within the bound.
A program may use at most 64 MiB of HBM per device.

```python
import math
import jax
import jax.numpy as jnp
import numpy as np
from jax import lax

D = 4096
HEADS = 32
HEAD_SIZE = 64
LAYERS = 2
POSITION = 2048
WIDTH = 2048
BATCH = 32


def draw_tokens(key, part):
    key_list = jax.random.split(key, 3)
    row_scale = jnp.exp(jax.random.uniform(key_list[0], (BATCH, 1), jnp.float32, math.log(0.3), math.log(3.0)))
    column_place = jnp.arange(D, dtype=jnp.float32) / D
    jitter = jnp.exp(jax.random.uniform(key_list[1], (1, D), jnp.float32, math.log(0.8), math.log(1.25)))
    column_scale = 0.5 * jnp.exp(column_place * math.log(4.0))[None, :] * jitter
    noise = jnp.clip(jax.random.normal(key_list[2], (BATCH, D), jnp.float32), -4.0, 4.0)
    return (noise * row_scale * column_scale).astype(jnp.bfloat16)


def shard_levels(key, dims, cuts, low, top_value):
    def one(axis_at, blocks):
        draws = jax.random.uniform(jax.random.fold_in(jax.random.fold_in(key, 6), axis_at), (blocks,), jnp.float32, low / len(cuts), top_value / len(cuts))
        return jnp.repeat(jnp.exp(draws), dims[axis_at] // blocks).reshape((-1,) + (1,) * (len(dims) - axis_at - 1))

    factor_of = one(*cuts[0])
    for cut in cuts[1:]:
        factor_of = factor_of * one(*cut)
    return factor_of


def split_up(amount, total, limit, slope):
    portions = [(1 << 20) // math.isqrt(grade ** slope) + 1 for grade in range(2, amount + 1)]
    surplus, holding = total - limit - (amount - 1), [1] * (amount - 1)
    while surplus > 0:
        movable = [i for i in range(amount - 1) if holding[i] < limit]
        whole, remaining = sum([portions[i] for i in movable]), surplus
        for i in movable:
            extra = min(limit - holding[i], max(1, remaining * portions[i] // whole), surplus)
            holding[i] = holding[i] + extra
            surplus = surplus - extra
    return np.array([limit] + holding)


def uneven(rng, amount, total, limit, skew):
    if amount == 2:
        one = jax.random.randint(rng, (), max(1, total - limit), min(limit, total - 1) + 1)
        return jnp.stack([one, total - one])
    sizes = jnp.asarray(split_up(amount, total, limit, skew), jnp.int32)
    twos = (amount - 1) // 2
    giver, receiver = sizes[1:1 + 2 * twos:2], sizes[2:2 + 2 * twos:2]
    room = jnp.minimum(giver - 1, limit - receiver)
    shifted = jax.random.randint(jax.random.fold_in(rng, 1), (twos,), 0, 1 << 20) % (room + 1)
    sizes = sizes.at[1:1 + 2 * twos:2].set(giver - shifted).at[2:2 + 2 * twos:2].set(receiver + shifted)
    return sizes[jax.random.permutation(jax.random.fold_in(rng, 2), amount)]


def centred(key, shape, scale, limit, pieces=(), held_as=jnp.bfloat16):
    result = scale * jax.random.normal(key, shape, jnp.float32)
    if pieces:
        result = result * shard_levels(key, shape, pieces, -0.22, 0.18)
    return jnp.clip(result, -limit, limit).astype(held_as)


def setup_inputs(seed: int = 0) -> dict:
    arg_keys = jax.random.split(jax.random.key(seed), 14)
    return {
        "tokens": draw_tokens(jax.random.fold_in(arg_keys[13], 71), 0),
        "lengths": uneven(arg_keys[1], BATCH, BATCH * POSITION, 4 * POSITION, 2).astype(jnp.int32),
        "in_gain": jnp.clip(1.0 + 0.18 * jax.random.normal(arg_keys[2], (LAYERS, D), jnp.float32), 0.1, 1.9),
        "w_recept": centred(arg_keys[3], (LAYERS, D, WIDTH), D ** -0.5, 0.09375, ((1, 4), (2, 8))),
        "w_key": centred(arg_keys[4], (LAYERS, D, WIDTH), D ** -0.5, 0.09375, ((1, 4), (2, 8))),
        "w_value": centred(arg_keys[5], (LAYERS, D, WIDTH), D ** -0.5, 0.09375, ((1, 4), (2, 8))),
        "w_decay": centred(arg_keys[6], (LAYERS, D, WIDTH), D ** -0.5, 0.09375, ((1, 4), (2, 8))),
        "w_rate": centred(arg_keys[7], (LAYERS, D, WIDTH), D ** -0.5, 0.09375, ((1, 4), (2, 8))),
        "w_gate": centred(arg_keys[8], (LAYERS, D, WIDTH), D ** -0.5, 0.09375, ((1, 4), (2, 8))),
        "w_out": centred(arg_keys[9], (LAYERS, WIDTH, D), WIDTH ** -0.5, 0.125, ((1, 8), (2, 4))),
        "decay_base": centred(arg_keys[10], (LAYERS, WIDTH), 2.0, 6.0, ((1, 8),), jnp.float32),
        "mix_gain": jnp.clip(1.0 + 0.18 * jax.random.normal(arg_keys[11], (LAYERS, WIDTH), jnp.float32), 0.1, 1.9),
        "states": centred(arg_keys[12], (LAYERS, BATCH, HEADS, HEAD_SIZE, HEAD_SIZE), 1.0, 6.0, ((1, 4), (2, 8)), jnp.float32),
    }


DECAY_SCALE = 0.6065306597126334
NORM_EPS = 1e-06
KEY_EPS = 1e-05
GROUP_EPS = 0.00064

def update_heads(projected, previous, base_row, gain_row, alive_rows):
    row_count = previous.shape[0]
    head_count = previous.shape[1]
    head_size = previous.shape[2]
    local_width = head_count * head_size
    role_parts = [projected[:, role_index * local_width:(role_index + 1) * local_width] for role_index in range(6)]
    recept, key_flat, value_flat, decay_pre, rate_pre, gate_pre = role_parts
    decay_factor = jnp.exp(-DECAY_SCALE * jax.nn.sigmoid(decay_pre + base_row))
    in_rate = jax.nn.sigmoid(rate_pre)
    key_heads = key_flat.reshape(row_count, head_count, head_size)
    unit_key = key_heads * lax.rsqrt(lax.optimization_barrier(jnp.sum(key_heads * key_heads, axis=2, keepdims=True)) + KEY_EPS)
    removed = jnp.einsum('bhvk,bhk->bhv', previous, -unit_key, precision=lax.Precision.HIGHEST)
    decay_heads = decay_factor.reshape(row_count, head_count, 1, head_size)
    rate_heads = in_rate.reshape(row_count, head_count, head_size)
    value_heads = value_flat.reshape(row_count, head_count, head_size)
    updated = previous * decay_heads + removed[..., None] * (unit_key * rate_heads)[:, :, None, :] + value_heads[..., None] * key_heads[:, :, None, :]
    recept_heads = recept.reshape(row_count, head_count, head_size)
    readout = jnp.einsum('bhvk,bhk->bhv', updated, recept_heads, precision=lax.Precision.HIGHEST)
    centre = lax.optimization_barrier(jnp.mean(readout, axis=2, keepdims=True))
    spread = lax.optimization_barrier(jnp.mean(jnp.square(readout - centre), axis=2, keepdims=True))
    normed = ((readout - centre) * lax.rsqrt(spread + GROUP_EPS)).reshape(row_count, local_width)
    normed = normed * gain_row * jax.nn.sigmoid(gate_pre)
    mixed_rows = jnp.where(alive_rows[:, None], normed, 0.0).astype(jnp.bfloat16)
    kept_state = jnp.where(alive_rows[:, None, None, None], updated, previous)
    return (mixed_rows, kept_state)

def reference(tokens, lengths, in_gain, w_recept, w_key, w_value, w_decay, w_rate, w_gate, w_out, decay_base, mix_gain, states):
    alive_rows = lengths > POSITION
    current = tokens
    kept_states = []
    for layer_index in range(LAYERS):
        widened = current.astype(jnp.float32)
        inverse = lax.rsqrt(lax.optimization_barrier(jnp.mean(widened * widened, axis=1, keepdims=True)) + NORM_EPS)
        scaled = (widened * in_gain[layer_index]).astype(jnp.bfloat16)
        outputs = [jnp.dot(scaled, weight[layer_index], preferred_element_type=jnp.float32) * inverse for weight in (w_recept, w_key, w_value, w_decay, w_rate, w_gate)]
        projected = jnp.concatenate(outputs, axis=1)
        mixed_rows, kept_state = update_heads(projected, states[layer_index], decay_base[layer_index], mix_gain[layer_index], alive_rows)
        branch = jnp.dot(mixed_rows, w_out[layer_index], preferred_element_type=jnp.float32)
        current = (widened + branch).astype(jnp.bfloat16)
        kept_states.append(kept_state)
    return (current, jnp.stack(kept_states))
```

```python
import functools

import jax
import jax.numpy as jnp
from jax import lax
from jax.experimental import pallas as pl
from jax.experimental.pallas import tpu as pltpu
from jax.sharding import PartitionSpec as P

POSITION = 2048
DECAY_SCALE = 0.6065306597126334
NORM_EPS = 1e-06
KEY_EPS = 1e-05
GROUP_EPS = 0.00064
ROLES = 6
GROUPS = 3
MESH = pl.DeviceIdType.MESH


def step_kernel(
    tp,
    dp,
    lengths_hbm,
    tokens,
    in_gain,
    decay_base,
    mix_gain,
    w_recept,
    w_key,
    w_value,
    w_decay,
    w_rate,
    w_gate,
    w_out,
    states,
    next_tokens,
    new_states,
    lengths,
    gain_v,
    base_v,
    mixgain_v,
    w_v,
    wo_v,
    xg,
    x32,
    psum,
    rbuf,
    vec,
    rows,
    mg,
    osum,
    obuf,
    small_sem,
    w_sem,
    wo_sem,
    s_sem,
    ag_s,
    ag_r,
    rs_s,
    rs_r,
    mg_s,
    mg_r,
    os_s,
    os_r,
):
    s_v = new_states
    layers, row_count, heads, size, _ = states.shape
    rt, cl = tokens.shape
    width = heads * size
    batch = rt * tp
    model = cl * dp
    me_tp = lax.axis_index("tp")
    me_dp = lax.axis_index("dp")
    far_first = sorted(range(1, tp), key=lambda k: -min(k, tp - k))
    tp_peers = [lax.rem(me_tp + k, tp) for k in far_first]
    dp_peers = [lax.rem(me_dp + k, dp) for k in range(1, dp)]

    tok_copy = pltpu.make_async_copy(tokens, xg.at[0, me_tp], small_sem.at[0])
    tok_copy.start()
    small = [
        pltpu.make_async_copy(in_gain, gain_v, small_sem.at[1]),
        pltpu.make_async_copy(decay_base, base_v, small_sem.at[2]),
        pltpu.make_async_copy(mix_gain, mixgain_v, small_sem.at[3]),
        pltpu.make_async_copy(lengths_hbm, lengths, small_sem.at[4]),
    ]
    for copy in small:
        copy.start()
    w_copies, wo_copies, s_copies = [], [], []
    for l in range(layers):
        per_role = []
        for r, w in enumerate((w_recept, w_key, w_value, w_decay, w_rate, w_gate)):
            per_role.append(pltpu.make_async_copy(w.at[l], w_v.at[l, r], w_sem.at[l, r]))
        w_copies.append(per_role)
        s_copies.append(pltpu.make_async_copy(states.at[l], s_v.at[l], s_sem.at[l]))
        wo_copies.append(pltpu.make_async_copy(w_out.at[l], wo_v.at[l], wo_sem.at[l]))
        for copy in per_role + [s_copies[l], wo_copies[l]]:
            copy.start()

    barrier = pltpu.get_barrier_semaphore()
    for peer in tp_peers:
        pl.semaphore_signal(barrier, inc=1, device_id={"tp": peer}, device_id_type=MESH)
    for peer in dp_peers:
        pl.semaphore_signal(barrier, inc=1, device_id={"dp": peer}, device_id_type=MESH)
    pl.semaphore_wait(barrier, tp - 1 + dp - 1)

    sends = []

    def exchange(src, dst, send_sem, recv_sem, axis, peer):
        copy = pltpu.make_async_remote_copy(
            src_ref=src,
            dst_ref=dst,
            send_sem=send_sem,
            recv_sem=recv_sem,
            device_id={axis: peer},
            device_id_type=MESH,
        )
        copy.start()
        sends.append(copy)
        return copy

    def gather_tokens(l):
        return [
            exchange(xg.at[l, me_tp], xg.at[l, me_tp], ag_s.at[l, k], ag_r.at[l, k], "tp", peer)
            for k, peer in enumerate(tp_peers)
        ]

    tok_copy.wait()
    incoming = gather_tokens(0)
    for copy in small:
        copy.wait()

    row_at = lax.broadcasted_iota(jnp.int32, (row_count, width), 0)
    len_rows = jnp.zeros((row_count, width), jnp.int32)
    for b in range(row_count):
        len_rows = jnp.where(row_at == b, lengths[b], len_rows)
    live_rows = len_rows > POSITION
    cube = (heads, size, size)
    eye = lax.broadcasted_iota(jnp.int32, cube, 1) == lax.broadcasted_iota(jnp.int32, cube, 2)

    for l in range(layers):
        for copy in incoming:
            copy.wait_recv()
        for i in range(tp):
            x32[i * rt : (i + 1) * rt, :] = xg[l, i].astype(jnp.float32)
        x = x32[...]
        squares = jnp.sum(x * x, axis=1, keepdims=True)
        spread_sq = jnp.broadcast_to(squares, (batch, width)).reshape(dp, row_count, width)
        coarse = spread_sq.astype(jnp.bfloat16)
        psum[l, :, 0] = coarse
        psum[l, :, 1] = (spread_sq - coarse.astype(jnp.float32)).astype(jnp.bfloat16)
        scaled = (x * gain_v[l : l + 1, :]).astype(jnp.bfloat16)
        incoming = []
        for r in range(ROLES):
            w_copies[l][r].wait()
            part = jnp.dot(scaled, w_v[l, r], preferred_element_type=jnp.float32)
            psum[l, :, r + 2] = part.reshape(dp, row_count, width).astype(jnp.bfloat16)
            if (r + 1) % (ROLES // GROUPS) == 0:
                g = r // (ROLES // GROUPS)
                lo = 0 if g == 0 else r + 3 - ROLES // GROUPS
                cut = pl.ds(lo, r + 3 - lo)
                for k, peer in enumerate(dp_peers):
                    incoming.append(
                        exchange(
                            psum.at[l, peer, cut],
                            rbuf.at[l, k, cut],
                            rs_s.at[l, g, k],
                            rs_r.at[l, g, k],
                            "dp",
                            peer,
                        )
                    )
        s_copies[l].wait()
        for copy in incoming:
            copy.wait_recv()
        total = []
        for r in range(ROLES + 2):
            plane = psum[l, me_dp, r].astype(jnp.float32)
            for k in range(dp - 1):
                plane = plane + rbuf[l, k, r].astype(jnp.float32)
            total.append(plane)
        inverse = lax.rsqrt((total[0] + total[1]) / model + NORM_EPS)
        recept, key, value, decay_pre, rate_pre, gate_pre = [plane * inverse for plane in total[2:]]
        decay = jnp.exp(-DECAY_SCALE * jax.nn.sigmoid(decay_pre + base_v[l : l + 1, :]))
        rate = jax.nn.sigmoid(rate_pre)
        offsets = []
        for h in range(heads):
            at = slice(h * size, (h + 1) * size)
            key_h, recept_h, decay_h, value_h = key[:, at], recept[:, at], decay[:, at], value[:, at]
            unit = key_h * lax.rsqrt(jnp.sum(key_h * key_h, axis=1, keepdims=True) + KEY_EPS)
            paced = unit * rate[:, at]
            along = jnp.sum(paced * recept_h, axis=1, keepdims=True)
            offsets.append(value_h * jnp.sum(key_h * recept_h, axis=1, keepdims=True))
            vec[0, h] = decay_h * recept_h - along * unit
            vec[1, h] = unit
            vec[2, h] = decay_h
            vec[3, h] = paced
            vec[4, h] = key_h
            vec[5, h] = value_h

        def read_row(b, carry, l=l):
            column = jnp.sum(s_v[l, b] * vec[0, :, pl.ds(b, 1), :], axis=2, keepdims=True)
            rows[:, pl.ds(b, 1), :] = jnp.sum(jnp.where(eye, column, 0.0), axis=1, keepdims=True)
            return carry

        lax.fori_loop(0, row_count, read_row, 0, unroll=True)
        pieces = []
        for h in range(heads):
            readout = rows[h] + offsets[h]
            moved = readout - jnp.mean(readout, axis=1, keepdims=True)
            spread = jnp.mean(moved * moved, axis=1, keepdims=True)
            pieces.append(moved * lax.rsqrt(spread + GROUP_EPS))
        normed = jnp.concatenate(pieces, axis=1) if heads > 1 else pieces[0]
        normed = normed * mixgain_v[l : l + 1, :] * jax.nn.sigmoid(gate_pre)
        mg[l, me_dp] = jnp.where(live_rows, normed, 0.0).astype(jnp.bfloat16)
        incoming = [
            exchange(mg.at[l, me_dp], mg.at[l, me_dp], mg_s.at[l, k], mg_r.at[l, k], "dp", peer)
            for k, peer in enumerate(dp_peers)
        ]

        def renew(b, carry, l=l):
            old = s_v[l, b]
            taken = jnp.sum(old * vec[1, :, pl.ds(b, 1), :], axis=2, keepdims=True)
            value_col = jnp.sum(jnp.where(eye, vec[5, :, pl.ds(b, 1), :], 0.0), axis=2, keepdims=True)
            fresh = (
                old * vec[2, :, pl.ds(b, 1), :]
                - taken * vec[3, :, pl.ds(b, 1), :]
                + value_col * vec[4, :, pl.ds(b, 1), :]
            )
            live = jnp.full(cube, lengths[b], jnp.int32) > POSITION
            s_v[l, b] = jnp.where(live, fresh, old)
            return carry

        lax.fori_loop(0, row_count, renew, 0, unroll=True)

        wo_copies[l].wait()
        for copy in incoming:
            copy.wait_recv()
        mixed = mg[l].astype(jnp.float32).reshape(batch, width).astype(jnp.bfloat16)
        terms = jnp.dot(mixed, wo_v[l], preferred_element_type=jnp.float32)
        for i in range(tp):
            osum[l, i] = terms[i * rt : (i + 1) * rt].astype(jnp.bfloat16)
        incoming = [
            exchange(osum.at[l, peer], obuf.at[l, k], os_s.at[l, k], os_r.at[l, k], "tp", peer)
            for k, peer in enumerate(tp_peers)
        ]
        branch = osum[l, me_tp].astype(jnp.float32)
        for k, copy in enumerate(incoming):
            copy.wait_recv()
            branch = branch + obuf[l, k].astype(jnp.float32)
        current = (xg[l, me_tp].astype(jnp.float32) + branch).astype(jnp.bfloat16)
        if l + 1 < layers:
            xg[l + 1, me_tp] = current
            incoming = gather_tokens(l + 1)
        else:
            next_tokens[...] = current

    for copy in sends:
        copy.wait_send()


def store_kernel(rows, held, next_tokens, new_states, sem):
    copies = [
        pltpu.make_async_copy(held, new_states, sem.at[0]),
        pltpu.make_async_copy(rows, next_tokens, sem.at[1]),
    ]
    for copy in copies:
        copy.start()
    for copy in copies:
        copy.wait()


def on_device(
    tokens,
    lengths,
    in_gain,
    w_recept,
    w_key,
    w_value,
    w_decay,
    w_rate,
    w_gate,
    w_out,
    decay_base,
    mix_gain,
    states,
):
    tp = lax.axis_size("tp")
    dp = lax.axis_size("dp")
    layers, row_count, heads, size, _ = states.shape
    rt, cl = tokens.shape
    width = heads * size
    batch = rt * tp
    f32, bf16 = jnp.float32, jnp.bfloat16
    hbm = pl.BlockSpec(memory_space=pltpu.HBM)
    vmem = pl.BlockSpec(memory_space=pltpu.VMEM)
    dma = pltpu.SemaphoreType.DMA
    held = pl.pallas_call(
        functools.partial(step_kernel, tp, dp),
        out_shape=(
            pltpu.VMEM(tokens.shape, tokens.dtype),
            pltpu.VMEM(states.shape, states.dtype),
        ),
        in_specs=[hbm] * 13,
        out_specs=(vmem, vmem),
        scratch_shapes=[
            pltpu.SMEM(lengths.shape, jnp.int32),
            pltpu.VMEM(in_gain.shape, f32),
            pltpu.VMEM(decay_base.shape, f32),
            pltpu.VMEM(mix_gain.shape, f32),
            pltpu.VMEM((layers, ROLES) + w_key.shape[1:], bf16),
            pltpu.VMEM(w_out.shape, bf16),
            pltpu.VMEM((layers, tp, rt, cl), bf16),
            pltpu.VMEM((batch, cl), f32),
            pltpu.VMEM((layers, dp, ROLES + 2, row_count, width), bf16),
            pltpu.VMEM((layers, dp - 1, ROLES + 2, row_count, width), bf16),
            pltpu.VMEM((6, heads, row_count, size), f32),
            pltpu.VMEM((heads, row_count, size), f32),
            pltpu.VMEM((layers, dp, row_count, width), bf16),
            pltpu.VMEM((layers, tp, rt, cl), bf16),
            pltpu.VMEM((layers, tp - 1, rt, cl), bf16),
            dma((5,)),
            dma((layers, ROLES)),
            dma((layers,)),
            dma((layers,)),
            dma((layers, tp - 1)),
            dma((layers, tp - 1)),
            dma((layers, GROUPS, dp - 1)),
            dma((layers, GROUPS, dp - 1)),
            dma((layers, dp - 1)),
            dma((layers, dp - 1)),
            dma((layers, tp - 1)),
            dma((layers, tp - 1)),
        ],
        compiler_params=pltpu.CompilerParams(
            collective_id=0, has_side_effects=True, vmem_limit_bytes=25165824
        ),
    )(*[pltpu.with_memory_space_constraint(x, pltpu.HBM) for x in (
        lengths,
        tokens,
        in_gain,
        decay_base,
        mix_gain,
        w_recept,
        w_key,
        w_value,
        w_decay,
        w_rate,
        w_gate,
        w_out,
        states,
    )])
    return pl.pallas_call(
        store_kernel,
        out_shape=(
            jax.ShapeDtypeStruct(tokens.shape, tokens.dtype),
            jax.ShapeDtypeStruct(states.shape, states.dtype),
        ),
        in_specs=[vmem, vmem],
        out_specs=(hbm, hbm),
        scratch_shapes=[dma((2,))],
        compiler_params=pltpu.CompilerParams(vmem_limit_bytes=1048576),
    )(*[pltpu.with_memory_space_constraint(x, pltpu.VMEM) for x in held])


def solution(mesh):
    in_specs = (
        P("tp", "dp"),
        P("dp"),
        P(None, "dp"),
        P(None, "dp", "tp"),
        P(None, "dp", "tp"),
        P(None, "dp", "tp"),
        P(None, "dp", "tp"),
        P(None, "dp", "tp"),
        P(None, "dp", "tp"),
        P(None, "tp", "dp"),
        P(None, "tp"),
        P(None, "tp"),
        P(None, "dp", "tp", None, None),
    )
    out_specs = (P("tp", "dp"), P(None, "dp", "tp", None, None))
    return jax.shard_map(
        on_device, mesh=mesh, in_specs=in_specs, out_specs=out_specs, check_vma=False
    )
```
